32 devices in a mesh: rep: 2 (over x), fs: 8 (over z, y), tp: 2 (over core).
Axes of the slice: x: 2, y: 2, z: 4, core: 2. Of those that a mesh axis runs over, the one named last changes fastest.
Arguments:
- tokens: bfloat16 [10240, 2048], P(('rep', 'fs', 'tp')), may hold values from -6 to 6
- mix_gain: float32 [2048], replicated, may hold values from 0.1 to 1.9
- w_bgate: bfloat16 [2048, 2048], P('fs', 'tp'), may hold values from -0.125 to 0.125
- w_cgate: bfloat16 [2048, 2048], P('fs', 'tp'), may hold values from -0.125 to 0.125
- w_value: bfloat16 [2048, 2048], P('fs', 'tp'), may hold values from -0.125 to 0.125
- conv_taps: float32 [3, 2048], replicated, may hold values from -3 to 3
- w_mixout: bfloat16 [2048, 2048], P('tp', 'fs'), may hold values from -0.125 to 0.125
- mlp_gain: float32 [2048], replicated, may hold values from 0.1 to 1.9
- w_gate: bfloat16 [2048, 2816], P('fs', 'tp'), may hold values from -0.125 to 0.125
- w_up: bfloat16 [2048, 2816], P('fs', 'tp'), may hold values from -0.125 to 0.125
- w_down: bfloat16 [2816, 2048], P('tp', 'fs'), may hold values from -0.109375 to 0.109375
Outputs:
- block_out: bfloat16 [10240, 2048], P(('rep', 'fs', 'tp'))
The draws below stay inside these ranges and needn't reach their ends.
All inputs are finite; a program needn't handle non-finite values.
Results may differ from the reference program's by a relative error of at most 0.0085.
Values may be sent and summed in bfloat16 or wider, within the bound.
No kernel may reach another device: no remote copies, remote signals or barrier semaphores. Data moves between devices by JAX's collectives and lax.ppermute only.
A program may use at most 128 MiB of HBM per device.

```python
import jax
import jax.numpy as jnp
from jax import lax

D = 2048
FF = 2816
LENGTH = 640
TOKENS = 10240
N_TP = 2


def block_scale(key, extent, split, least, top_value):
    level, own = 1.0, jax.random.fold_in(key, 6)
    for dim, blocks in split:
        steps = jnp.exp(jax.random.uniform(jax.random.fold_in(own, dim), (blocks,), jnp.float32, least / len(split), top_value / len(split)))
        level = level * jnp.repeat(steps, extent[dim] // blocks).reshape([-1 if axis == dim else 1 for axis in range(len(extent))])
    return level


def centred(own_key, extent, width, bound, cuts=(), dtype=jnp.bfloat16):
    drawn = jax.random.normal(own_key, extent, jnp.float32) * width
    if len(cuts) > 0:
        drawn = block_scale(own_key, extent, cuts, -0.22, 0.18) * drawn
    return jnp.clip(drawn, min=-bound, max=bound).astype(dtype)


def setup_inputs(seed: int = 0) -> dict:
    key_of = jax.random.split(jax.random.key(seed), 12)
    tokens = centred(key_of[0], (TOKENS, D), 1.0, 6.0, ((0, 32),))
    mix_gain = jnp.clip(1.0 + 0.18 * jax.random.normal(key_of[1], (D,), jnp.float32), 0.1, 1.9)
    w_bgate = centred(key_of[2], (D, D), D ** -0.5, 0.125, ((0, 8), (1, 2)))
    w_cgate = centred(key_of[3], (D, D), D ** -0.5, 0.125, ((0, 8), (1, 2)))
    w_value = centred(key_of[4], (D, D), D ** -0.5, 0.125, ((0, 8), (1, 2)))
    conv_taps = centred(key_of[5], (3, D), 0.6, 3.0, (), jnp.float32)
    w_mixout = centred(key_of[6], (D, D), D ** -0.5, 0.125, ((0, 2), (1, 8)))
    mlp_gain = jnp.clip(1.0 + 0.18 * jax.random.normal(key_of[7], (D,), jnp.float32), 0.1, 1.9)
    w_gate = centred(key_of[8], (D, FF), D ** -0.5, 0.125, ((0, 8), (1, 2)))
    w_up = centred(key_of[9], (D, FF), D ** -0.5, 0.125, ((0, 8), (1, 2)))
    w_down = centred(key_of[10], (FF, D), FF ** -0.5, 0.109375, ((0, 2), (1, 8)))
    return {"tokens": tokens, "mix_gain": mix_gain, "w_bgate": w_bgate, "w_cgate": w_cgate, "w_value": w_value, "conv_taps": conv_taps, "w_mixout": w_mixout, "mlp_gain": mlp_gain, "w_gate": w_gate, "w_up": w_up, "w_down": w_down}


def rms_scale(matrix, gain):
    values = matrix.astype(jnp.float32)
    factor = lax.rsqrt(lax.optimization_barrier(jnp.mean(values * values, axis=-1, keepdims=True)) + 1e-06)
    return values * factor * gain.astype(jnp.float32)

def causal_taps(mixed, filters):
    length = mixed.shape[-2]
    widths = [(0, 0)] * (mixed.ndim - 2) + [(2, 0), (0, 0)]
    padded = jnp.pad(mixed, widths)
    return filters[0] * padded[..., 0:length, :] + filters[1] * padded[..., 1:length + 1, :] + filters[2] * padded[..., 2:length + 2, :]

def split_sum(left, right):
    portion = left.shape[1] // N_TP
    running = jnp.zeros((left.shape[0], right.shape[1]), jnp.float32)
    for member in range(N_TP):
        partial_out = jnp.dot(left[:, member * portion:(member + 1) * portion], right[member * portion:(member + 1) * portion], preferred_element_type=jnp.float32)
        partial_out = lax.optimization_barrier(partial_out.astype(jnp.bfloat16))
        running = running + partial_out.astype(jnp.float32)
    return running

def reference(tokens, mix_gain, w_bgate, w_cgate, w_value, conv_taps, w_mixout, mlp_gain, w_gate, w_up, w_down):
    normed = rms_scale(tokens, mix_gain).astype(jnp.bfloat16)
    b_proj = jnp.dot(normed, w_bgate, preferred_element_type=jnp.float32).astype(jnp.bfloat16)
    c_proj = jnp.dot(normed, w_cgate, preferred_element_type=jnp.float32).astype(jnp.bfloat16)
    u_proj = jnp.dot(normed, w_value, preferred_element_type=jnp.float32).astype(jnp.bfloat16)
    mixed_in = c_proj.astype(jnp.float32) * u_proj.astype(jnp.float32)
    mixed_in = mixed_in.reshape(TOKENS // LENGTH, LENGTH, D)
    convolved = causal_taps(mixed_in, conv_taps).reshape(TOKENS, D)
    gated = (b_proj.astype(jnp.float32) * convolved).astype(jnp.bfloat16)
    residual = tokens.astype(jnp.float32) + split_sum(gated, w_mixout)
    normed_two = rms_scale(residual, mlp_gain).astype(jnp.bfloat16)
    gate = jnp.dot(normed_two, w_gate, preferred_element_type=jnp.float32)
    up_value = jnp.dot(normed_two, w_up, preferred_element_type=jnp.float32)
    hidden = (jax.nn.silu(gate) * up_value).astype(jnp.bfloat16)
    return (residual + 0.5 * split_sum(hidden, w_down)).astype(jnp.bfloat16)
```

```python
import functools

import jax
import jax.numpy as jnp
from jax import lax
from jax.experimental import pallas as pl
from jax.experimental.pallas import tpu as pltpu
from jax.sharding import PartitionSpec as P


LANES = 128
TILE = 256
F32 = jnp.float32
BF16 = jnp.bfloat16
ANY = pl.BlockSpec(memory_space=pl.ANY)
VMEM = pl.BlockSpec(memory_space=pltpu.VMEM)


def rms_scale(matrix, gain):
    values = matrix.astype(F32)
    factor = lax.rsqrt(jnp.mean(values * values, axis=-1, keepdims=True) + 1e-06)
    return values * factor * gain


def causal_taps(mixed, filters):
    length = mixed.shape[-2]
    widths = [(0, 0)] * (mixed.ndim - 2) + [(2, 0), (0, 0)]
    padded = jnp.pad(mixed, widths)
    return (
        filters[0] * padded[..., 0:length, :]
        + filters[1] * padded[..., 1 : length + 1, :]
        + filters[2] * padded[..., 2 : length + 2, :]
    )


def gather_rows(normed):
    return lax.all_gather(normed, "tp", axis=0, tiled=True)


def project_in(gathered, stacked):
    return jnp.einsum(
        "td,kdc->ktc",
        gathered,
        lax.all_gather(stacked, "fs", axis=1, tiled=True),
        preferred_element_type=F32,
    )


def collect_out(weight):
    return lax.all_gather(weight, "fs", axis=1, tiled=True)


def sum_parts(local_cols, weight):
    return lax.psum_scatter(
        jnp.dot(local_cols, weight, preferred_element_type=F32).astype(BF16),
        "tp",
        scatter_dimension=0,
        tiled=True,
    ).astype(F32)


def plain(
    tokens, mix_gain, w_bgate, w_cgate, w_value, conv_taps, w_mixout, mlp_gain, w_gate, w_up, w_down
):
    normed = rms_scale(tokens, mix_gain).astype(BF16)
    gathered = gather_rows(normed)
    projected = project_in(gathered, jnp.stack([w_bgate, w_cgate, w_value])).astype(BF16)
    channels = projected.shape[2]
    channel_taps = lax.dynamic_slice_in_dim(conv_taps, lax.axis_index("tp") * channels, channels, 1)
    mixed_in = projected[1].astype(F32) * projected[2].astype(F32)
    gated = (projected[0].astype(F32) * causal_taps(mixed_in, channel_taps)).astype(BF16)
    residual = tokens.astype(F32) + sum_parts(gated, collect_out(w_mixout))
    normed_two = rms_scale(residual, mlp_gain).astype(BF16)
    gathered_two = gather_rows(normed_two)
    gate_up = project_in(gathered_two, jnp.stack([w_gate, w_up]))
    hidden = (jax.nn.silu(gate_up[0]) * gate_up[1]).astype(BF16)
    result = residual + 0.5 * sum_parts(hidden, collect_out(w_down))
    return result.astype(BF16)


def flip(value, mask):
    bit = 1
    while bit <= mask:
        if mask & bit:
            value = value + bit - 2 * bit * (lax.div(value, bit) - 2 * lax.div(value, 2 * bit))
        bit *= 2
    return value


def place():
    fs = lax.axis_index("fs")
    return lax.axis_index("rep"), lax.div(fs, 2), lax.rem(fs, 2), lax.axis_index("tp")


def to_rep(value):
    return lax.ppermute(value, "rep", [(0, 1), (1, 0)])


def to_tp(value):
    return lax.ppermute(value, "tp", [(0, 1), (1, 0)])


class Moves:
    def __init__(self, shards):
        self.shards = shards
        self.lines = shards // 2

    def to_pair(self, value):
        return lax.ppermute(value, "fs", [(f, f ^ 1) for f in range(self.shards)])

    def along(self, value, moves):
        return lax.ppermute(value, "fs", [(2 * a + p, 2 * b + p) for a, b in moves for p in (0, 1)])

    def slots(self, value):
        lines = range(self.lines)
        found = []
        for mask in range(1, self.lines):
            if self.lines == 4 and mask == 3:
                inner = self.along(value, [(1, 2), (2, 1)])
                outer = self.along(found[1], [(2, 3), (1, 0)])
                line = place()[1]
                found.append(jnp.where((line == 1) | (line == 2), inner, outer))
            else:
                found.append(self.along(value, [(a, a ^ mask) for a in lines]))
        return found


def after(value, *others):
    return lax.optimization_barrier((value, *others))[0]


def half_of(columns):
    half = -(-columns // (2 * LANES)) * LANES
    return half, 2 * half - columns


def cut_in(weights, pair, rep):
    rows, columns = weights[0].shape
    half, over = half_of(columns)
    return jnp.stack(
        [
            lax.dynamic_slice(w, (rep * (rows // 2), pair * (half - over)), (rows // 2, half))
            for w in weights
        ]
    )


def fill(copies, sems):
    started = [
        pltpu.make_async_copy(source, target, sems.at[index])
        for index, (source, target) in enumerate(copies)
    ]
    for copy in started:
        copy.start()
    return started


def token_copies(refs, buffer, rows):
    tp = lax.axis_index("tp")
    return [
        (ref, buffer.at[seq, pl.ds(pl.multiple_of(core * rows, rows), rows), :])
        for ref, (seq, core) in zip(refs, ((0, tp), (0, 1 - tp), (1, tp), (1, 1 - tp)))
    ]


def in_copies(own_refs, pieces, refs, buffer):
    rep, line, pair, _ = place()
    shard_rows, columns = own_refs[0].shape
    half, over = half_of(columns)
    piece_rows = shard_rows // 2
    copies = []
    for index, ref in enumerate(own_refs):
        start = pl.multiple_of((line * 2 + pair) * shard_rows, shard_rows)
        offset = pl.multiple_of(pair * (half - over), LANES)
        copies.append(
            (ref.at[:, pl.ds(offset, half)], buffer.at[index, pl.ds(start, shard_rows), :])
        )
    for ref, (lead, mask, other_pair, other_rep) in zip(refs, pieces):
        owner = flip(line, mask) * 2 + (1 - pair if other_pair else pair)
        part = 1 - rep if other_rep else rep
        start = pl.multiple_of(owner * shard_rows + part * piece_rows, piece_rows)
        source = ref if lead is None else ref.at[lead]
        copies.append((source, buffer.at[:, pl.ds(start, piece_rows), :]))
    return copies


def out_copies(own_ref, pieces, refs, buffer):
    rep, line, pair, _ = place()
    depth, columns = own_ref.shape
    half = depth // 2
    copies = [
        (own_ref, buffer.at[:, pl.ds(pl.multiple_of((line * 2 + pair) * columns, columns), columns)])
    ]
    for ref, (mask, other_pair, part) in zip(refs, pieces):
        owner = flip(line, mask) * 2 + (1 - pair if other_pair else pair)
        start = pl.multiple_of(owner * columns, columns)
        if part is None:
            target = buffer.at[:, pl.ds(start, columns)]
        else:
            row = pl.multiple_of((1 - rep if part else rep) * half, half)
            target = buffer.at[pl.ds(row, half), pl.ds(start, columns)]
        copies.append((ref, target))
    return copies


def shifted(values, steps):
    moved = pltpu.roll(values, steps, 0)
    row = lax.broadcasted_iota(jnp.int32, values.shape, 0)
    return jnp.where(row >= steps, moved, 0.0)


def mixer_kernel(n_in, pieces, taps_ref, *refs):
    token_refs, own_refs, refs = refs[:4], refs[4 : 4 + n_in], refs[4 + n_in :]
    piece_refs, refs = refs[: len(pieces)], refs[len(pieces) :]
    keep_ref, send_ref, x, w, res, sems, out_sems = refs
    rows = token_refs[0].shape[0]
    _, _, pair, tp = place()
    half = res.shape[2]
    copies = token_copies(token_refs, x, rows) + in_copies(own_refs, pieces, piece_refs, w)
    for copy in fill(copies, sems):
        copy.wait()
    tiles = half // TILE

    def step(index, _):
        seq = 1 - lax.div(index, tiles)
        start = pl.multiple_of(lax.rem(index, tiles) * TILE, TILE)
        cols = pl.ds(start, TILE)
        xs = x[seq]
        c = jnp.dot(xs, w[0, :, cols], preferred_element_type=F32).astype(BF16).astype(F32)
        u = jnp.dot(xs, w[1, :, cols], preferred_element_type=F32).astype(BF16).astype(F32)
        mixed = c * u
        channel = pl.multiple_of(tp * (2 * half) + pair * half + start, LANES)
        taps = taps_ref[:, pl.ds(channel, TILE)]
        conv = taps[0:1] * shifted(mixed, 2) + taps[1:2] * shifted(mixed, 1) + taps[2:3] * mixed
        b = jnp.dot(xs, w[2, :, cols], preferred_element_type=F32).astype(BF16).astype(F32)
        res[seq, :, cols] = (b * conv).astype(BF16)
        return 0

    lax.fori_loop(0, 2 * tiles, step, 0)
    outs = fill([(res.at[1], send_ref), (res.at[0], keep_ref)], out_sems)
    for copy in outs:
        copy.wait()


def hidden_kernel(n_in, pieces, *refs):
    token_refs, own_refs, refs = refs[:4], refs[4 : 4 + n_in], refs[4 + n_in :]
    piece_refs, refs = refs[: len(pieces)], refs[len(pieces) :]
    keep_ref, send_ref, x, w, res, sems, out_sems = refs
    rows = token_refs[0].shape[0]
    pair = place()[2]
    half, over = half_of(own_refs[0].shape[1])
    copies = token_copies(token_refs, x, rows) + in_copies(own_refs, pieces, piece_refs, w)
    for copy in fill(copies, sems):
        copy.wait()
    tiles = half // TILE

    def step(index, _):
        seq = 1 - lax.div(index, tiles)
        cols = pl.ds(pl.multiple_of(lax.rem(index, tiles) * TILE, TILE), TILE)
        xs = x[seq]
        gate = jnp.dot(xs, w[0, :, cols], preferred_element_type=F32)
        up = jnp.dot(xs, w[1, :, cols], preferred_element_type=F32)
        res[seq, :, cols] = (gate / (1.0 + jnp.exp(-gate)) * up).astype(BF16)
        return 0

    lax.fori_loop(0, 2 * tiles, step, 0)
    first = pl.multiple_of(pair * over, LANES)
    outs = fill(
        [(res.at[1, :, pl.ds(first, half - over)], send_ref), (res.at[0], keep_ref)], out_sems
    )
    for copy in outs:
        copy.wait()


def out_kernel(pieces, keep_in, recv_in, own_ref, *refs):
    piece_refs, refs = refs[: len(pieces)], refs[len(pieces) :]
    keep_ref, send_ref, left, w, res, sems, out_sems = refs
    _, _, pair, tp = place()
    half, over = half_of(left.shape[1])
    main = half - over
    copies = [
        (
            keep_in.at[:, pl.ds(pl.multiple_of(pair * over, LANES), main)],
            left.at[:, pl.ds(pl.multiple_of(pair * half, LANES), main)],
        ),
        (recv_in, left.at[:, pl.ds(pl.multiple_of((1 - pair) * half, LANES), main)]),
    ]
    if over:
        copies.append(
            (
                keep_in.at[:, pl.ds(pl.multiple_of((1 - pair) * main, LANES), over)],
                left.at[:, pl.ds(main, over)],
            )
        )
    copies += out_copies(own_ref, pieces, piece_refs, w)
    for copy in fill(copies, sems):
        copy.wait()

    def step(index, _):
        cols = pl.ds(pl.multiple_of(index * TILE, TILE), TILE)
        res[:, cols] = jnp.dot(left[...], w[:, cols], preferred_element_type=F32).astype(BF16)
        return 0

    lax.fori_loop(0, w.shape[1] // TILE, step, 0)
    rows = keep_ref.shape[0]
    mine = pl.ds(pl.multiple_of(tp * rows, rows), rows)
    theirs = pl.ds(pl.multiple_of((1 - tp) * rows, rows), rows)
    outs = fill([(res.at[theirs, :], send_ref), (res.at[mine, :], keep_ref)], out_sems)
    for copy in outs:
        copy.wait()


def cost(arrays, flops, transcendentals=0):
    size = sum(a.size * a.dtype.itemsize for a in arrays)
    return pl.CostEstimate(flops=flops, bytes_accessed=size, transcendentals=transcendentals)


def shape(*dims, dtype=BF16):
    return jax.ShapeDtypeStruct(dims, dtype)


def mixer(taps, token_parts, own, pieces, arrays):
    rows, depth = token_parts[0].shape
    half, _ = half_of(own[0].shape[1])
    copies = 4 + len(own) + len(pieces)
    out = shape(2 * rows, half)
    return pl.pallas_call(
        functools.partial(mixer_kernel, len(own), pieces),
        out_shape=(out, out),
        in_specs=[VMEM] + [ANY] * copies,
        out_specs=(ANY, ANY),
        scratch_shapes=[
            pltpu.VMEM((2, 2 * rows, depth), BF16),
            pltpu.VMEM((len(own), depth, half), BF16),
            pltpu.VMEM((2, 2 * rows, half), BF16),
            pltpu.SemaphoreType.DMA((copies,)),
            pltpu.SemaphoreType.DMA((2,)),
        ],
        compiler_params=pltpu.CompilerParams(vmem_limit_bytes=48 << 20),
        cost_estimate=cost(token_parts + arrays, 2 * 4 * rows * depth * half * len(own)),
        name="mixer",
    )(taps, *token_parts, *own, *arrays)


def hidden_of(token_parts, own, pieces, arrays):
    rows, depth = token_parts[0].shape
    half, over = half_of(own[0].shape[1])
    copies = 4 + len(own) + len(pieces)
    return pl.pallas_call(
        functools.partial(hidden_kernel, len(own), pieces),
        out_shape=(shape(2 * rows, half), shape(2 * rows, half - over)),
        in_specs=[ANY] * copies,
        out_specs=(ANY, ANY),
        scratch_shapes=[
            pltpu.VMEM((2, 2 * rows, depth), BF16),
            pltpu.VMEM((len(own), depth, half), BF16),
            pltpu.VMEM((2, 2 * rows, half), BF16),
            pltpu.SemaphoreType.DMA((copies,)),
            pltpu.SemaphoreType.DMA((2,)),
        ],
        compiler_params=pltpu.CompilerParams(vmem_limit_bytes=48 << 20),
        cost_estimate=cost(token_parts + arrays, 2 * 4 * rows * depth * half * len(own)),
        name="hidden",
    )(*token_parts, *own, *arrays)


def out_of(keep, recv, own, pieces, arrays, width):
    length = keep.shape[0]
    depth = own.shape[0]
    _, over = half_of(depth)
    copies = 2 + (over > 0) + 1 + len(pieces)
    return pl.pallas_call(
        functools.partial(out_kernel, pieces),
        out_shape=(shape(length // 2, width), shape(length // 2, width)),
        in_specs=[ANY] * (3 + len(pieces)),
        out_specs=(ANY, ANY),
        scratch_shapes=[
            pltpu.VMEM((length, depth), BF16),
            pltpu.VMEM((depth, width), BF16),
            pltpu.VMEM((length, width), BF16),
            pltpu.SemaphoreType.DMA((copies,)),
            pltpu.SemaphoreType.DMA((2,)),
        ],
        compiler_params=pltpu.CompilerParams(vmem_limit_bytes=48 << 20),
        cost_estimate=cost([keep, recv] + arrays, 2 * length * depth * width),
        name="project_out",
    )(keep, recv, own, *arrays)


def norm_kernel(tokens_ref, gain_ref, out_ref):
    values = tokens_ref[...].astype(F32)
    factor = lax.rsqrt(jnp.mean(values * values, axis=-1, keepdims=True) + 1e-06)
    out_ref[...] = (values * factor * gain_ref[...]).astype(BF16)


def residual_kernel(tokens_ref, keep_ref, recv_ref, gain_ref, residual_ref, out_ref):
    values = tokens_ref[...].astype(F32) + (keep_ref[...].astype(F32) + recv_ref[...].astype(F32))
    residual_ref[...] = values
    factor = lax.rsqrt(jnp.mean(values * values, axis=-1, keepdims=True) + 1e-06)
    out_ref[...] = (values * factor * gain_ref[...]).astype(BF16)


def by_rows(kernel, arrays, gain, dtypes):
    rows, width = arrays[0].shape
    step = next(s for s in (80, 64, 32, 16, 8) if rows % s == 0)
    block = pl.BlockSpec((step, width), lambda i: (i, 0))
    outs = tuple(shape(rows, width, dtype=d) for d in dtypes)
    return pl.pallas_call(
        kernel,
        grid=(rows // step,),
        out_shape=outs,
        in_specs=[block] * len(arrays) + [pl.BlockSpec((1, width), lambda i: (0, 0))],
        out_specs=(block,) * len(outs),
        compiler_params=pltpu.CompilerParams(vmem_limit_bytes=16 << 20),
        cost_estimate=cost(arrays + list(outs), 8 * rows * width),
        name="norm",
    )(*arrays, gain.reshape(1, width))


def share(moves, own):
    mine = to_tp(own)
    far = moves.to_pair(own)
    return [own, mine, far, to_tp(far)]


def on_device(
    moves, tokens, mix_gain, w_bgate, w_cgate, w_value, conv_taps, w_mixout, mlp_gain, w_gate, w_up, w_down
):
    rep, line, pair, tp = place()
    width = tokens.shape[1]
    first = [w_cgate, w_value, w_bgate]
    second = [w_gate, w_up]
    masks = range(1, moves.lines)

    mine = cut_in(first, pair, rep)
    far = moves.to_pair(cut_in(first, 1 - pair, rep))
    (normed,) = by_rows(norm_kernel, [tokens], mix_gain, [BF16])
    token_parts = share(moves, normed)
    near_slots = moves.slots(mine)
    far_slots = moves.slots(far)
    pieces, arrays = [(None, 0, 1, 0), (None, 0, 1, 1)], [far, to_rep(far)]
    for mask, a, b in zip(masks, near_slots, far_slots):
        pieces += [(None, mask, 0, 0), (None, mask, 0, 1), (None, mask, 1, 0), (None, mask, 1, 1)]
        arrays += [a, to_rep(a), b, to_rep(b)]
    keep, send = mixer(conv_taps, token_parts, first, pieces, arrays)

    depth, columns = w_mixout.shape
    cut = lax.dynamic_slice(w_mixout, (rep * (depth // 2), 0), (depth // 2, columns))
    slots = moves.slots(after(cut, near_slots[-1]))
    pieces, arrays = [(0, 1, None)], [moves.to_pair(w_mixout)]
    for mask, a in zip(masks, slots):
        b = to_rep(a)
        pieces += [(mask, 0, 0), (mask, 0, 1), (mask, 1, 0), (mask, 1, 1)]
        arrays += [a, b, moves.to_pair(a), moves.to_pair(b)]
    mix_keep, mix_send = out_of(keep, moves.to_pair(send), w_mixout, pieces, arrays, width)
    mix_slots = slots

    theirs = moves.to_pair(after(cut_in(second, 1 - pair, rep), far))
    both = after(jnp.stack([cut_in(second, pair, rep), theirs]), far_slots[-1])
    slots = moves.slots(both)
    pieces, arrays = [(None, 0, 1, 0), (None, 0, 1, 1)], [theirs, to_rep(theirs)]
    for mask, a in zip(masks, slots):
        b = to_rep(a)
        pieces += [(0, mask, 0, 0), (0, mask, 0, 1), (1, mask, 1, 0), (1, mask, 1, 1)]
        arrays += [a, b, a, b]
    residual, normed_two = by_rows(
        residual_kernel, [tokens, mix_keep, to_tp(mix_send)], mlp_gain, [F32, BF16]
    )
    keep, send = hidden_of(share(moves, normed_two), second, pieces, arrays)

    depth, columns = w_down.shape
    cut = lax.dynamic_slice(w_down, (rep * (depth // 2), 0), (depth // 2, columns))
    cut = after(cut, mix_slots[-1])
    down_slots = moves.slots(cut)
    pair_cut = moves.to_pair(cut)
    pieces, arrays = [(0, 1, 0), (0, 1, 1)], [pair_cut, to_rep(pair_cut)]
    for mask, a in zip(masks, down_slots):
        b = moves.to_pair(a)
        pieces += [(mask, 0, 0), (mask, 0, 1), (mask, 1, 0), (mask, 1, 1)]
        arrays += [a, to_rep(a), b, to_rep(b)]
    down_keep, down_send = out_of(keep, moves.to_pair(send), w_down, pieces, arrays, width)
    down_sum = down_keep.astype(F32) + to_tp(down_send).astype(F32)
    return (residual + 0.5 * down_sum).astype(BF16)


def fits(mesh):
    shards = mesh.shape["fs"]
    lines = shards // 2
    even = mesh.shape["rep"] == 2 and mesh.shape["tp"] == 2 and shards % 2 == 0
    return even and lines >= 1 and lines & (lines - 1) == 0


def tiles(shards, tokens, w_cgate, w_mixout, w_gate, w_down):
    rows, columns = w_cgate.shape
    half, over = half_of(columns)
    checks = [rows % 32, tokens.shape[0] % 16, half % TILE, over]
    half, over = half_of(w_gate.shape[1])
    checks += [half % TILE, tokens.shape[1] % TILE]
    for w in (w_mixout, w_down):
        checks += [w.shape[0] % 32, w.shape[1] % LANES]
    return not any(checks)


def solution(mesh):
    def program(*args):
        tokens, _, _, w_cgate, _, _, w_mixout, _, w_gate, _, w_down = args
        moves = Moves(mesh.shape["fs"])
        if fits(mesh) and tiles(moves.shards, tokens, w_cgate, w_mixout, w_gate, w_down):
            return on_device(moves, *args)
        return plain(*args)

    return jax.shard_map(
        program,
        mesh=mesh,
        in_specs=(
            P(("rep", "fs", "tp"), None),
            P(),
            P("fs", "tp"),
            P("fs", "tp"),
            P("fs", "tp"),
            P(),
            P("tp", "fs"),
            P(),
            P("fs", "tp"),
            P("fs", "tp"),
            P("tp", "fs"),
        ),
        out_specs=P(("rep", "fs", "tp"), None),
        check_vma=False,
    )
```

```python
import functools

import jax
import jax.numpy as jnp
from jax import lax
from jax.experimental import pallas as pl
from jax.experimental.pallas import tpu as pltpu
from jax.sharding import PartitionSpec as P


LANES = 128
TILE = 256
F32 = jnp.float32
BF16 = jnp.bfloat16
HBM = pl.BlockSpec(memory_space=pltpu.HBM)
VMEM = pl.BlockSpec(memory_space=pltpu.VMEM)


def rms_scale(matrix, gain):
    values = matrix.astype(F32)
    factor = lax.rsqrt(jnp.mean(values * values, axis=-1, keepdims=True) + 1e-06)
    return values * factor * gain


def causal_taps(mixed, filters):
    length = mixed.shape[-2]
    widths = [(0, 0)] * (mixed.ndim - 2) + [(2, 0), (0, 0)]
    padded = jnp.pad(mixed, widths)
    return (
        filters[0] * padded[..., 0:length, :]
        + filters[1] * padded[..., 1 : length + 1, :]
        + filters[2] * padded[..., 2 : length + 2, :]
    )


def gather_rows(normed):
    return lax.all_gather(normed, "tp", axis=0, tiled=True)


def project_all(gathered, stacked):
    return jnp.einsum(
        "td,kdc->ktc",
        gathered,
        lax.all_gather(stacked, "fs", axis=1, tiled=True),
        preferred_element_type=F32,
    )


def collect_out(weight):
    return lax.all_gather(weight, "fs", axis=1, tiled=True)


def sum_parts(local_cols, weight):
    return lax.psum_scatter(
        jnp.dot(local_cols, weight, preferred_element_type=F32).astype(BF16),
        "tp",
        scatter_dimension=0,
        tiled=True,
    ).astype(F32)


def plain(
    tokens, mix_gain, w_bgate, w_cgate, w_value, conv_taps, w_mixout, mlp_gain, w_gate, w_up, w_down
):
    normed = rms_scale(tokens, mix_gain).astype(BF16)
    gathered = gather_rows(normed)
    projected = project_all(gathered, jnp.stack([w_bgate, w_cgate, w_value])).astype(BF16)
    channels = projected.shape[2]
    channel_taps = lax.dynamic_slice_in_dim(conv_taps, lax.axis_index("tp") * channels, channels, 1)
    mixed_in = projected[1].astype(F32) * projected[2].astype(F32)
    gated = (projected[0].astype(F32) * causal_taps(mixed_in, channel_taps)).astype(BF16)
    residual = tokens.astype(F32) + sum_parts(gated, collect_out(w_mixout))
    normed_two = rms_scale(residual, mlp_gain).astype(BF16)
    gathered_two = gather_rows(normed_two)
    gate_up = project_all(gathered_two, jnp.stack([w_gate, w_up]))
    hidden = (jax.nn.silu(gate_up[0]) * gate_up[1]).astype(BF16)
    result = residual + 0.5 * sum_parts(hidden, collect_out(w_down))
    return result.astype(BF16)


def flip(value, mask):
    bit = 1
    while bit <= mask:
        if mask & bit:
            value = value + bit - 2 * bit * (lax.div(value, bit) - 2 * lax.div(value, 2 * bit))
        bit *= 2
    return value


def place():
    fs = lax.axis_index("fs")
    return lax.axis_index("rep"), lax.div(fs, 2), lax.rem(fs, 2), lax.axis_index("tp")


def to_rep(value):
    return lax.ppermute(value, "rep", [(0, 1), (1, 0)])


def to_tp(value):
    return lax.ppermute(value, "tp", [(0, 1), (1, 0)])


class Moves:
    def __init__(self, shards):
        self.shards = shards
        self.lines = shards // 2

    def to_pair(self, value):
        return lax.ppermute(value, "fs", [(f, f ^ 1) for f in range(self.shards)])

    def along(self, value, moves):
        pairs = [(2 * a + p, 2 * b + p) for a, b in moves for p in (0, 1)]
        return lax.ppermute(value, "fs", pairs)

    def slots(self, value, whole=None, relay=False):
        four = self.lines == 4
        line = place()[1]
        middle = (line == 1) | (line == 2)
        inner, outer = [(1, 2), (2, 1)], [(2, 3), (1, 0)]
        if four and relay:
            near = self.along(value, [(a, a ^ 1) for a in range(4)])
            b = self.along(value, inner)
            c = self.along(near, inner)
            d = self.along(b, outer)
            e = self.along(c, outer)
            return [near, jnp.where(middle, c, d), jnp.where(middle, b, e)]
        found = []
        for mask in range(1, self.lines):
            sent = value if whole is None or mask > 2 else whole
            if four and mask == 3:
                own = self.along(value, inner)
                passed = found[1]
                if whole is not None:
                    passed = rep_half(passed)
                found.append(jnp.where(middle, own, self.along(passed, outer)))
            else:
                found.append(self.along(sent, [(a, a ^ mask) for a in range(self.lines)]))
        return found


def rep_half(weight):
    half = weight.shape[0] // 2
    return lax.dynamic_slice(weight, (place()[0] * half, 0), (half, weight.shape[1]))


def half_of(columns):
    half = -(-columns // (2 * LANES)) * LANES
    return half, 2 * half - columns


def cut_in(weights, pair, rep):
    rows, columns = weights[0].shape
    half, over = half_of(columns)
    return jnp.stack(
        [
            lax.dynamic_slice(w, (rep * (rows // 2), pair * (half - over)), (rows // 2, half))
            for w in weights
        ]
    )


def token_copies(refs, buffer, rows):
    tp = lax.axis_index("tp")
    return [
        (ref, buffer.at[pl.ds(pl.multiple_of(core * rows, rows), rows), :])
        for ref, core in zip(refs, (tp, 1 - tp))
    ]


def in_copies(own_refs, pieces, refs, buffer, tile):
    rep, line, pair, _ = place()
    shard_rows, columns = own_refs[0].shape
    half, over = half_of(columns)
    piece_rows = shard_rows // 2
    cols = pl.ds(tile * TILE, TILE)
    copies = []
    for index, ref in enumerate(own_refs):
        start = pl.multiple_of((line * 2 + pair) * shard_rows, shard_rows)
        offset = pl.multiple_of(pair * (half - over) + tile * TILE, LANES)
        copies.append(
            (ref.at[:, pl.ds(offset, TILE)], buffer.at[index, pl.ds(start, shard_rows), cols])
        )
    for ref, (lead, mask, other_pair, other_rep) in zip(refs, pieces):
        owner = flip(line, mask) * 2 + (1 - pair if other_pair else pair)
        part = 1 - rep if other_rep else rep
        start = pl.multiple_of(owner * shard_rows + part * piece_rows, piece_rows)
        source = ref.at[:, :, cols] if lead is None else ref.at[lead, :, :, cols]
        copies.append((source, buffer.at[:, pl.ds(start, piece_rows), cols]))
    return copies


def launch(copies, sem):
    for source, target in copies:
        pltpu.make_async_copy(source, target, sem).start()


def await_all(target, sem):
    pltpu.make_async_copy(target, target, sem).wait()


def shifted(values, steps):
    moved = pltpu.roll(values, steps, 0)
    row = lax.broadcasted_iota(jnp.int32, values.shape, 0)
    return jnp.where(row >= steps, moved, 0.0)


def in_kernel(n_in, pieces, tile_of, sent, *refs):
    extra, refs = refs[0], refs[1:]
    token_refs, own_refs, refs = refs[:2], refs[2 : 2 + n_in], refs[2 + n_in :]
    piece_refs, refs = refs[: len(pieces)], refs[len(pieces) :]
    out_ref, x, w, res, x_sem, w_sems, out_sem = refs
    half = res.shape[1]
    tiles = half // TILE
    launch(token_copies(token_refs, x, token_refs[0].shape[0]), x_sem)
    for tile in range(tiles):
        launch(in_copies(own_refs, pieces, piece_refs, w, tile), w_sems.at[tile])
    await_all(x, x_sem)

    def step(tile, _):
        cols = pl.ds(pl.multiple_of(tile * TILE, TILE), TILE)
        await_all(w.at[:, :, cols], w_sems.at[tile])
        res[:, cols] = tile_of(x, w, extra, cols, tile)
        return 0

    lax.fori_loop(0, tiles, step, 0)
    source = res
    if sent:
        over = half - out_ref.shape[1]
        source = res.at[:, pl.ds(pl.multiple_of(place()[2] * over, LANES), half - over)]
    copy = pltpu.make_async_copy(source, out_ref, out_sem)
    copy.start()
    copy.wait()


def gated_tile(x, w, taps_ref, cols, tile):
    _, _, pair, tp = place()
    half = w.shape[2]
    xs = x[...]
    c = jnp.dot(xs, w[0, :, cols], preferred_element_type=F32).astype(BF16).astype(F32)
    u = jnp.dot(xs, w[1, :, cols], preferred_element_type=F32).astype(BF16).astype(F32)
    mixed = c * u
    channel = pl.multiple_of(tp * (2 * half) + pair * half + tile * TILE, LANES)
    taps = taps_ref[:, pl.ds(channel, TILE)]
    conv = taps[0:1] * shifted(mixed, 2) + taps[1:2] * shifted(mixed, 1) + taps[2:3] * mixed
    b = jnp.dot(xs, w[2, :, cols], preferred_element_type=F32).astype(BF16).astype(F32)
    return (b * conv).astype(BF16)


def hidden_tile(x, w, _, cols, tile):
    xs = x[...]
    gate = jnp.dot(xs, w[0, :, cols], preferred_element_type=F32)
    up = jnp.dot(xs, w[1, :, cols], preferred_element_type=F32)
    return (gate / (1.0 + jnp.exp(-gate)) * up).astype(BF16)


def out_kernel(pieces, shards, keep_in, recv_in, own_ref, *refs):
    piece_refs, refs = refs[: len(pieces)], refs[len(pieces) :]
    keep_ref, send_ref, left, w, res, left_sem, w_sems, out_sems = refs
    rep, line, pair, tp = place()
    depth, columns = own_ref.shape
    half, over = half_of(depth)
    main = half - over
    copies = [
        (
            keep_in.at[:, pl.ds(pl.multiple_of(pair * over, LANES), main)],
            left.at[:, pl.ds(pl.multiple_of(pair * half, LANES), main)],
        ),
        (recv_in, left.at[:, pl.ds(pl.multiple_of((1 - pair) * half, LANES), main)]),
    ]
    if over:
        copies.append(
            (
                keep_in.at[:, pl.ds(pl.multiple_of((1 - pair) * main, LANES), over)],
                left.at[:, pl.ds(main, over)],
            )
        )
    launch(copies, left_sem)

    launch([(own_ref, w.at[0])], w_sems.at[0])
    by_block = sorted(zip(pieces, piece_refs), key=lambda item: item[0][:2])
    for (mask, other_pair, part), ref in by_block:
        block = 2 * mask + other_pair
        if part is None:
            target = w.at[block]
        else:
            row = pl.multiple_of((1 - rep if part else rep) * (depth // 2), depth // 2)
            target = w.at[block, pl.ds(row, depth // 2)]
        launch([(ref, target)], w_sems.at[block])
    await_all(left, left_sem)
    rows = keep_ref.shape[0]
    mine = pl.ds(pl.multiple_of(tp * rows, rows), rows)
    theirs = pl.ds(pl.multiple_of((1 - tp) * rows, rows), rows)

    def step(block, _):
        await_all(w.at[block], w_sems.at[block])
        mask, other = lax.div(block, 2), lax.rem(block, 2)
        owner, bit = 0, 1
        while bit < shards // 2:
            owner += bit * lax.rem(lax.div(line, bit) + lax.div(mask, bit), 2)
            bit *= 2
        owner = 2 * owner + lax.rem(pair + other, 2)
        cols = pl.ds(pl.multiple_of(owner * columns, columns), columns)
        res[:, cols] = jnp.dot(left[...], w[block], preferred_element_type=F32).astype(BF16)
        launch([(res.at[theirs, cols], send_ref.at[:, cols])], out_sems.at[0])
        launch([(res.at[mine, cols], keep_ref.at[:, cols])], out_sems.at[1])
        return 0

    lax.fori_loop(0, shards, step, 0)
    await_all(send_ref, out_sems.at[0])
    await_all(keep_ref, out_sems.at[1])


def cost(arrays, flops, transcendentals=0):
    size = sum(a.size * a.dtype.itemsize for a in arrays)
    return pl.CostEstimate(flops=flops, bytes_accessed=size, transcendentals=transcendentals)


def shape(*dims, dtype=BF16):
    return jax.ShapeDtypeStruct(dims, dtype)


def kernel_call(kernel, **options):
    def call(*args):
        return pl.pallas_call(kernel, **options)(*args)

    return call


def project_in(tile_of, extra, tokens, own, pieces, arrays, sent):
    rows, depth = tokens[0].shape
    half, over = half_of(own[0].shape[1])
    width = half - over if sent else half
    return kernel_call(
        functools.partial(in_kernel, len(own), pieces, tile_of, sent),
        out_shape=shape(2 * rows, width),
        in_specs=[VMEM] + [HBM] * (2 + len(own) + len(pieces)),
        out_specs=HBM,
        scratch_shapes=[
            pltpu.VMEM((2 * rows, depth), BF16),
            pltpu.VMEM((len(own), depth, half), BF16),
            pltpu.VMEM((2 * rows, half), BF16),
            pltpu.SemaphoreType.DMA,
            pltpu.SemaphoreType.DMA((half // TILE,)),
            pltpu.SemaphoreType.DMA,
        ],
        compiler_params=pltpu.CompilerParams(vmem_limit_bytes=40 << 20),
        cost_estimate=cost(tokens + arrays, 4 * rows * depth * half * len(own)),
    )(extra, *tokens, *own, *arrays)


def project_out(shards, keep, recv, own, pieces, arrays):
    length = keep.shape[0]
    depth, columns = own.shape
    width = shards * columns
    return kernel_call(
        functools.partial(out_kernel, pieces, shards),
        out_shape=(shape(length // 2, width), shape(length // 2, width)),
        in_specs=[HBM] * (3 + len(pieces)),
        out_specs=(HBM, HBM),
        scratch_shapes=[
            pltpu.VMEM((length, depth), BF16),
            pltpu.VMEM((shards, depth, columns), BF16),
            pltpu.VMEM((length, width), BF16),
            pltpu.SemaphoreType.DMA,
            pltpu.SemaphoreType.DMA((shards,)),
            pltpu.SemaphoreType.DMA((2,)),
        ],
        compiler_params=pltpu.CompilerParams(vmem_limit_bytes=40 << 20),
        cost_estimate=cost([keep, recv] + arrays, 2 * length * depth * width),
    )(keep, recv, own, *arrays)


def norm_kernel(tokens_ref, gain_ref, out_ref):
    values = tokens_ref[...].astype(F32)
    factor = lax.rsqrt(jnp.mean(values * values, axis=-1, keepdims=True) + 1e-06)
    out_ref[...] = (values * factor * gain_ref[...]).astype(BF16)


def residual_kernel(tokens_ref, keep_ref, recv_ref, gain_ref, residual_ref, out_ref):
    values = tokens_ref[...].astype(F32) + (keep_ref[...].astype(F32) + recv_ref[...].astype(F32))
    residual_ref[...] = values
    factor = lax.rsqrt(jnp.mean(values * values, axis=-1, keepdims=True) + 1e-06)
    out_ref[...] = (values * factor * gain_ref[...]).astype(BF16)


def final_kernel(residual_ref, keep_ref, recv_ref, _, out_ref):
    down_sum = keep_ref[...].astype(F32) + recv_ref[...].astype(F32)
    out_ref[...] = (residual_ref[...] + 0.5 * down_sum).astype(BF16)


def by_rows(kernel, arrays, gain, dtypes):
    rows, width = arrays[0].shape
    step = next(s for s in (80, 64, 32, 16, 8) if rows % s == 0)
    block = pl.BlockSpec((step, width), lambda i: (i, 0))
    outs = tuple(shape(rows, width, dtype=d) for d in dtypes)
    return kernel_call(
        kernel,
        grid=(rows // step,),
        out_shape=outs,
        in_specs=[block] * len(arrays) + [pl.BlockSpec((1, width), lambda i: (0, 0))],
        out_specs=(block,) * len(outs),
        compiler_params=pltpu.CompilerParams(vmem_limit_bytes=16 << 20),
        cost_estimate=cost(arrays + list(outs), 8 * rows * width),
    )(*arrays, gain.reshape(1, width))


def share(moves, own):
    mine = to_tp(own)
    far = moves.to_pair(own)
    return [own, mine, far, to_tp(far)]


def on_device(
    moves, tokens, mix_gain, w_bgate, w_cgate, w_value, conv_taps, w_mixout, mlp_gain, w_gate, w_up, w_down
):
    rep, _, pair, _ = place()
    first = [w_cgate, w_value, w_bgate]
    second = [w_gate, w_up]
    masks = range(1, moves.lines)

    mine = cut_in(first, pair, rep)
    far = moves.to_pair(cut_in(first, 1 - pair, rep))
    (normed,) = by_rows(norm_kernel, [tokens], mix_gain, [BF16])
    token_parts = share(moves, normed)
    near_slots = moves.slots(mine, relay=True)
    far_slots = moves.slots(far, relay=True)
    pieces, arrays = [(None, 0, 1, 0), (None, 0, 1, 1)], [far, to_rep(far)]
    for mask, a, b in zip(masks, near_slots, far_slots):
        pieces += [(None, mask, 0, 0), (None, mask, 0, 1), (None, mask, 1, 0), (None, mask, 1, 1)]
        arrays += [a, to_rep(a), b, to_rep(b)]
    send = project_in(gated_tile, conv_taps, token_parts[2:], first, pieces, arrays, True)
    keep = project_in(gated_tile, conv_taps, token_parts[:2], first, pieces, arrays, False)

    slots = moves.slots(rep_half(w_mixout))
    pieces, arrays = [(0, 1, None)], [moves.to_pair(w_mixout)]
    for mask, a in zip(masks, slots):
        b = to_rep(a)
        pieces += [(mask, 0, 0), (mask, 0, 1), (mask, 1, 0), (mask, 1, 1)]
        arrays += [a, b, moves.to_pair(a), moves.to_pair(b)]
    recv = moves.to_pair(send)
    mix_keep, mix_send = project_out(moves.shards, keep, recv, w_mixout, pieces, arrays)

    theirs = moves.to_pair(cut_in(second, 1 - pair, rep))
    slots = moves.slots(jnp.stack([cut_in(second, pair, rep), theirs]), relay=True)
    pieces, arrays = [(None, 0, 1, 0), (None, 0, 1, 1)], [theirs, to_rep(theirs)]
    for mask, a in zip(masks, slots):
        b = to_rep(a)
        pieces += [(0, mask, 0, 0), (0, mask, 0, 1), (1, mask, 1, 0), (1, mask, 1, 1)]
        arrays += [a, b, a, b]
    residual, normed_two = by_rows(
        residual_kernel, [tokens, mix_keep, to_tp(mix_send)], mlp_gain, [F32, BF16]
    )
    token_parts = share(moves, normed_two)
    keep = project_in(hidden_tile, conv_taps, token_parts[:2], second, pieces, arrays, False)
    send = project_in(hidden_tile, conv_taps, token_parts[2:], second, pieces, arrays, True)

    cut = rep_half(w_down)
    slots = moves.slots(cut, whole=w_down)
    pair_cut = moves.to_pair(cut)
    pieces, arrays = [(0, 1, 0), (0, 1, 1)], [pair_cut, to_rep(pair_cut)]
    for mask, a in zip(masks, slots):
        if mask > 2:
            pieces += [(mask, 0, 0), (mask, 0, 1)]
            arrays += [a, to_rep(a)]
        else:
            pieces.append((mask, 0, None))
            arrays.append(a)
            a = rep_half(a)
        b = moves.to_pair(a)
        pieces += [(mask, 1, 0), (mask, 1, 1)]
        arrays += [b, to_rep(b)]
    recv = moves.to_pair(send)
    down_keep, down_send = project_out(moves.shards, keep, recv, w_down, pieces, arrays)
    (result,) = by_rows(final_kernel, [residual, down_keep, to_tp(down_send)], mlp_gain, [BF16])
    return result


def fits(mesh):
    shards = mesh.shape["fs"]
    lines = shards // 2
    even = mesh.shape["rep"] == 2 and mesh.shape["tp"] == 2 and shards % 2 == 0
    return even and lines >= 1 and lines & (lines - 1) == 0


def tiles(tokens, w_cgate, w_mixout, w_gate, w_down):
    rows, columns = w_cgate.shape
    half, over = half_of(columns)
    checks = [rows % 32, tokens.shape[0] % 16, half % TILE, over]
    half, over = half_of(w_gate.shape[1])
    checks += [half % TILE, tokens.shape[1] % TILE]
    for w in (w_mixout, w_down):
        checks += [w.shape[0] % 32, w.shape[1] % LANES]
    return not any(checks)


def solution(mesh):
    def program(*args):
        tokens, _, _, w_cgate, _, _, w_mixout, _, w_gate, _, w_down = args
        moves = Moves(mesh.shape["fs"])
        if fits(mesh) and tiles(tokens, w_cgate, w_mixout, w_gate, w_down):
            return on_device(moves, *args)
        return plain(*args)

    return jax.shard_map(
        program,
        mesh=mesh,
        in_specs=(
            P(("rep", "fs", "tp"), None),
            P(),
            P("fs", "tp"),
            P("fs", "tp"),
            P("fs", "tp"),
            P(),
            P("tp", "fs"),
            P(),
            P("fs", "tp"),
            P("fs", "tp"),
            P("tp", "fs"),
        ),
        out_specs=P(("rep", "fs", "tp"), None),
        check_vma=False,
    )
```
